32 devices in a mesh: sp: 8 (over z, x), tp: 4 (over y, core).
Axes of the slice: x: 2, y: 2, z: 4, core: 2. Of those that a mesh axis runs over, the one named last changes fastest.
Arguments:
- residual: bfloat16 [2048, 2048], P('sp', 'tp'), may hold values from -8 to 8
- query_latent: bfloat16 [2048, 512], P('sp'), may hold values from -6 to 6
- shared_latent: bfloat16 [2048, 256], P('sp'), may hold values from -6 to 6
- rotary_key: bfloat16 [2048, 32], P('sp'), may hold values from -300 to 300
- query_gain: float32 [512], replicated, may hold values from 0.1 to 1.9
- latent_gain: float32 [256], replicated, may hold values from 0.1 to 1.9
- query_narrow: bfloat16 [512, 384], P(None, 'tp'), may hold values from -0.5 to 0.5
- key_narrow: bfloat16 [256, 256], P(None, 'tp'), may hold values from -0.375 to 0.375
- value_narrow: bfloat16 [256, 256], P(None, 'tp'), may hold values from -0.375 to 0.375
- query_wide: bfloat16 [512, 640], P(None, 'tp'), may hold values from -0.5 to 0.5
- key_wide: bfloat16 [256, 512], P(None, 'tp'), may hold values from -0.375 to 0.375
- value_wide: bfloat16 [256, 512], P(None, 'tp'), may hold values from -0.375 to 0.375
- output_narrow: bfloat16 [256, 2048], P('tp'), may hold values from -1.75 to 1.75
- output_wide: bfloat16 [512, 2048], P('tp'), may hold values from -1.75 to 1.75
- first_gain: float32 [2048], P('tp'), may hold values from 0.1 to 1.9
- first_bias: float32 [2048], P('tp'), may hold values from -1.5 to 1.5
- gate_weight: bfloat16 [2048, 5632], P('sp', 'tp'), may hold values from -0.125 to 0.125
- up_weight: bfloat16 [2048, 5632], P('sp', 'tp'), may hold values from -0.125 to 0.125
- down_weight: bfloat16 [5632, 2048], P('tp', 'sp'), may hold values from -0.078125 to 0.078125
- second_gain: float32 [2048], P('tp'), may hold values from 0.1 to 1.9
- second_bias: float32 [2048], P('tp'), may hold values from -1.5 to 1.5
Outputs:
- layer_out: bfloat16 [2048, 2048], P('sp', 'tp')
The draws below stay inside these ranges and needn't reach their ends.
All inputs are finite; a program needn't handle non-finite values.
Results may differ from the reference program's by a relative error of at most 0.017.
The reference program's roundings to bfloat16 on the way count: a program that leaves them out, or rounds other values in their place, can miss the bound.
Values may be sent and summed in bfloat16 or wider, within the bound.
No kernel may reach another device: no remote copies, remote signals or barrier semaphores. Data moves between devices by JAX's collectives and lax.ppermute only.
A program may use at most 192 MiB of HBM per device.

```python
import math
import jax
import jax.numpy as jnp
from jax import lax

D = 2048
FF = 5632
QL = 512
KVL = 256
ROPE = 32
HEADS_A = 4
HEADS_B = 4
NOPE_A = 64
V_A = 64
NOPE_B = 128
V_B = 128
GRID_W = 64
TOKENS = 2048


def draw_residual(key, part):
    col_scale = jnp.exp(jnp.linspace(math.log(0.5), math.log(1.5), D))
    base = jax.random.normal(key, (TOKENS, D), dtype=jnp.float32) * col_scale
    return jnp.clip(base, -8.0, 8.0).astype(jnp.bfloat16)


def draw_rotary_key(key, part):
    base = jax.random.normal(key, (TOKENS, ROPE), dtype=jnp.float32)
    return jnp.clip(base, -300.0, 300.0).astype(jnp.bfloat16)


def block_levels(stream_key, shape, cuts, least, high):
    level = 1.0
    for dim, blocks in cuts:
        steps = jax.random.uniform(jax.random.fold_in(jax.random.fold_in(stream_key, 6), dim), (blocks,), jnp.float32, least / len(cuts), high / len(cuts))
        level = level * jnp.repeat(jnp.exp(steps), shape[dim] // blocks).reshape((-1,) + (1,) * (len(shape) - 1 - dim))
    return level


def bell_draw(rng, dims, scale, most, shards=(), kind=jnp.bfloat16):
    result = scale * jax.random.normal(rng, dims, jnp.float32)
    if shards:
        result = result * block_levels(rng, dims, shards, -0.22, 0.18)
    return jnp.clip(result, -most, most).astype(kind)


def setup_inputs(seed: int = 0) -> dict:
    seeds = jax.random.split(jax.random.key(seed), 22)
    return {
        "residual": draw_residual(jax.random.fold_in(seeds[21], 71), 0),
        "query_latent": bell_draw(seeds[1], (TOKENS, QL), 1.0, 6.0, ((0, 8),)),
        "shared_latent": bell_draw(seeds[2], (TOKENS, KVL), 1.0, 6.0, ((0, 8),)),
        "rotary_key": draw_rotary_key(jax.random.fold_in(seeds[21], 71), 0),
        "query_gain": jnp.clip(1.0 + 0.18 * jax.random.normal(seeds[4], (QL,), jnp.float32), 0.1, 1.9),
        "latent_gain": jnp.clip(1.0 + 0.18 * jax.random.normal(seeds[5], (KVL,), jnp.float32), 0.1, 1.9),
        "query_narrow": bell_draw(seeds[6], (QL, HEADS_A * (NOPE_A + ROPE)), (QL // 4) ** -0.5, 0.5, ((1, 4),)),
        "key_narrow": bell_draw(seeds[7], (KVL, HEADS_A * NOPE_A), KVL ** -0.5, 0.375, ((1, 4),)),
        "value_narrow": bell_draw(seeds[8], (KVL, HEADS_A * V_A), KVL ** -0.5, 0.375, ((1, 4),)),
        "query_wide": bell_draw(seeds[9], (QL, HEADS_B * (NOPE_B + ROPE)), (QL // 4) ** -0.5, 0.5, ((1, 4),)),
        "key_wide": bell_draw(seeds[10], (KVL, HEADS_B * NOPE_B), KVL ** -0.5, 0.375, ((1, 4),)),
        "value_wide": bell_draw(seeds[11], (KVL, HEADS_B * V_B), KVL ** -0.5, 0.375, ((1, 4),)),
        "output_narrow": bell_draw(seeds[12], (HEADS_A * V_A, D), ((HEADS_A * V_A + HEADS_B * V_B) // 64) ** -0.5, 1.75, ((0, 4),)),
        "output_wide": bell_draw(seeds[13], (HEADS_B * V_B, D), ((HEADS_A * V_A + HEADS_B * V_B) // 64) ** -0.5, 1.75, ((0, 4),)),
        "first_gain": jnp.clip(1.0 + 0.18 * jax.random.normal(seeds[14], (D,), jnp.float32), 0.1, 1.9),
        "first_bias": bell_draw(seeds[15], (D,), 0.3, 1.5, ((0, 4),), jnp.float32),
        "gate_weight": bell_draw(seeds[16], (D, FF), D ** -0.5, 0.125, ((0, 8), (1, 4))),
        "up_weight": bell_draw(seeds[17], (D, FF), D ** -0.5, 0.125, ((0, 8), (1, 4))),
        "down_weight": bell_draw(seeds[18], (FF, D), FF ** -0.5, 0.078125, ((0, 4), (1, 8))),
        "second_gain": jnp.clip(1.0 + 0.18 * jax.random.normal(seeds[19], (D,), jnp.float32), 0.1, 1.9),
        "second_bias": bell_draw(seeds[20], (D,), 0.3, 1.5, ((0, 4),), jnp.float32),
    }


EPS_ROOT = 1e-06
EPS_LAYER = 1e-05
THETA = 10000.0
DEEP_ALPHA = 2.0 ** 0.25

def rotate(half_part, angle):
    lower, upper = jnp.split(half_part, 2, axis=-1)
    cosine = jnp.cos(angle)
    sine = jnp.sin(angle)
    return jnp.concatenate([lower * cosine - upper * sine, upper * cosine + lower * sine], axis=-1)

def turn_axial(values_in, positions):
    quarter = values_in.shape[-1] // 4
    freqs = THETA ** (-(2.0 * jnp.arange(quarter, dtype=jnp.float32)) / (2 * quarter))
    row_angle = (positions // GRID_W).astype(jnp.float32)[:, None, None] * freqs
    col_angle = (positions % GRID_W).astype(jnp.float32)[:, None, None] * freqs
    first_half, second_half = jnp.split(values_in, 2, axis=-1)
    return jnp.concatenate([rotate(first_half, row_angle), rotate(second_half, col_angle)], axis=-1)

def root_scale(latent, gain):
    floated = latent.astype(jnp.float32)
    return floated * lax.rsqrt(lax.optimization_barrier(jnp.mean(floated * floated, axis=-1, keepdims=True)) + EPS_ROOT) * gain.astype(jnp.float32)

def make_query(normed, weight, plain_dim, positions):
    product = jnp.dot(normed, weight, preferred_element_type=jnp.float32)
    head_count = weight.shape[1] // (plain_dim + ROPE)
    product = product.reshape(product.shape[0], head_count, plain_dim + ROPE)
    turned = turn_axial(product[:, :, plain_dim:], positions)
    return jnp.concatenate([product[:, :, :plain_dim], turned], axis=-1).astype(jnp.bfloat16)

def attend(queries, key_rows, value_rows, rotary_rows, plain_dim):
    count, head_count, query_dim = queries.shape
    block_size = math.gcd(count, 512)
    score_scale = query_dim ** (-0.5)
    key_float = key_rows.astype(jnp.float32)
    value_float = value_rows.astype(jnp.float32)
    rotary_float = rotary_rows.astype(jnp.float32)

    def per_block(query_block):
        query_float = query_block.astype(jnp.float32)
        scores = jnp.einsum('qhd,khd->hqk', query_float[:, :, :plain_dim], key_float)
        scores = (scores + jnp.einsum('qhd,kd->hqk', query_float[:, :, plain_dim:], rotary_float)) * score_scale
        largest = lax.optimization_barrier(jnp.max(scores, axis=-1, keepdims=True))
        raised = jnp.exp(scores - largest)
        totals = lax.optimization_barrier(jnp.sum(raised, axis=-1))
        rounded = lax.optimization_barrier(raised.astype(jnp.bfloat16)).astype(jnp.float32)
        output = jnp.einsum('hqk,khd->qhd', rounded, value_float) / totals.T[:, :, None]
        return output.astype(jnp.bfloat16)
    blocks = lax.map(per_block, queries.reshape(count // block_size, block_size, head_count, query_dim))
    return blocks.reshape(count, head_count * value_rows.shape[2])

def layer_norm(summed, gain, bias):
    center = lax.optimization_barrier(jnp.mean(summed, axis=-1, keepdims=True))
    spread = lax.optimization_barrier(jnp.mean((summed - center) * (summed - center), axis=-1, keepdims=True))
    normed = (summed - center) * lax.rsqrt(spread + EPS_LAYER) * gain.astype(jnp.float32) + bias.astype(jnp.float32)
    return normed.astype(jnp.bfloat16)

def reference(residual, query_latent, shared_latent, rotary_key, query_gain, latent_gain, query_narrow, key_narrow, value_narrow, query_wide, key_wide, value_wide, output_narrow, output_wide, first_gain, first_bias, gate_weight, up_weight, down_weight, second_gain, second_bias):
    positions = jnp.arange(residual.shape[0], dtype=jnp.int32)
    query_normed = root_scale(query_latent, query_gain).astype(jnp.bfloat16)
    latent_normed = root_scale(shared_latent, latent_gain).astype(jnp.bfloat16)
    rotary_rows = turn_axial(rotary_key.astype(jnp.float32)[:, None, :], positions)[:, 0, :].astype(jnp.bfloat16)

    def group(query_weight, key_weight, value_weight, plain_dim, value_dim):
        queries = make_query(query_normed, query_weight, plain_dim, positions)
        head_count = queries.shape[1]
        key_rows = jnp.dot(latent_normed, key_weight, preferred_element_type=jnp.float32).astype(jnp.bfloat16)
        value_rows = jnp.dot(latent_normed, value_weight, preferred_element_type=jnp.float32).astype(jnp.bfloat16)
        key_rows = key_rows.reshape(key_rows.shape[0], head_count, plain_dim)
        value_rows = value_rows.reshape(value_rows.shape[0], head_count, value_dim)
        return attend(queries, key_rows, value_rows, rotary_rows, plain_dim)
    attended_narrow = group(query_narrow, key_narrow, value_narrow, NOPE_A, V_A)
    attended_wide = group(query_wide, key_wide, value_wide, NOPE_B, V_B)
    mixed = jnp.dot(attended_narrow, output_narrow, preferred_element_type=jnp.float32)
    mixed = mixed + jnp.dot(attended_wide, output_wide, preferred_element_type=jnp.float32)
    normed_first = layer_norm(DEEP_ALPHA * residual.astype(jnp.float32) + mixed, first_gain, first_bias)
    gate = jnp.dot(normed_first, gate_weight, preferred_element_type=jnp.float32)
    lifted = jnp.dot(normed_first, up_weight, preferred_element_type=jnp.float32)
    hidden = (jax.nn.silu(gate) * lifted).astype(jnp.bfloat16)
    feed = jnp.dot(hidden, down_weight, preferred_element_type=jnp.float32)
    return layer_norm(DEEP_ALPHA * normed_first.astype(jnp.float32) + feed, second_gain, second_bias)
```

```python
import jax
import jax.numpy as jnp
from jax import lax
from jax.sharding import PartitionSpec as P

ROPE = 32
NOPE_A = 64
NOPE_B = 128
GRID_W = 64


EPS_ROOT = 1e-06
EPS_LAYER = 1e-05
THETA = 10000.0
DEEP_ALPHA = 2.0**0.25


def rotate(half_part, angle):
    lower, upper = jnp.split(half_part, 2, axis=-1)
    cosine = jnp.cos(angle)
    sine = jnp.sin(angle)
    return jnp.concatenate([lower * cosine - upper * sine, upper * cosine + lower * sine], axis=-1)


def turn_axial(values_in, positions):
    quarter = values_in.shape[-1] // 4
    freqs = THETA ** (-(2.0 * jnp.arange(quarter, dtype=jnp.float32)) / (2 * quarter))
    row_angle = (positions // GRID_W).astype(jnp.float32)[:, None, None] * freqs
    col_angle = (positions % GRID_W).astype(jnp.float32)[:, None, None] * freqs
    first_half, second_half = jnp.split(values_in, 2, axis=-1)
    return jnp.concatenate([rotate(first_half, row_angle), rotate(second_half, col_angle)], axis=-1)


def root_scale(latent, gain):
    floated = latent.astype(jnp.float32)
    return (
        floated * lax.rsqrt(jnp.mean(floated * floated, axis=-1, keepdims=True) + EPS_ROOT) * gain
    )


def make_query(normed, weight, plain_dim, positions):
    product = jnp.dot(normed, weight, preferred_element_type=jnp.float32)
    head_count = weight.shape[1] // (plain_dim + ROPE)
    product = product.reshape(product.shape[0], head_count, plain_dim + ROPE)
    turned = turn_axial(product[:, :, plain_dim:], positions)
    return jnp.concatenate([product[:, :, :plain_dim], turned], axis=-1).astype(jnp.bfloat16)


def attend(queries, keys, values, rotated, plain_dim):
    score_scale = queries.shape[2] ** (-0.5)
    scores = jnp.einsum(
        "qhd,khd->hqk", queries[:, :, :plain_dim], keys, preferred_element_type=jnp.float32
    )
    scores = scores + jnp.einsum(
        "qhd,kd->hqk", queries[:, :, plain_dim:], rotated, preferred_element_type=jnp.float32
    )
    scores = scores * score_scale
    largest = jnp.max(scores, axis=-1, keepdims=True)
    raised = jnp.exp(scores - largest)
    totals = jnp.sum(raised, axis=-1)
    weighted = jnp.einsum(
        "hqk,khd->qhd", raised.astype(jnp.bfloat16), values, preferred_element_type=jnp.float32
    )
    output = (weighted / totals.T[:, :, None]).astype(jnp.bfloat16)
    return output.reshape(output.shape[0], output.shape[1] * output.shape[2])


def swap(value, axis, bit):
    count = lax.axis_size(axis)
    return lax.ppermute(value, axis, [(i, i ^ bit) for i in range(count)])


def tp_bits():
    bits = []
    bit = 1
    while bit < lax.axis_size("tp"):
        bits.append(bit)
        bit *= 2
    return bits


def gather_blocks(own):
    blocks = {0: own}
    for bit in reversed(tp_bits()):
        for q in list(blocks):
            blocks[q ^ bit] = swap(blocks[q], "tp", bit)
    return blocks


def fold_tp(blocks, bits):
    for bit in bits:
        sent = [q for q in sorted(blocks) if q & bit]
        packed = jnp.concatenate([blocks[q].astype(jnp.bfloat16) for q in sent], axis=1)
        got = swap(packed, "tp", bit)
        width = got.shape[1] // len(sent)
        blocks = {
            q ^ bit: blocks[q ^ bit]
            + got[:, n * width : (n + 1) * width].astype(jnp.float32)
            for n, q in enumerate(sent)
        }
    return blocks


def layer_stats(summed):
    stats = jnp.stack([jnp.sum(summed, axis=1), jnp.sum(summed * summed, axis=1)])
    total = lax.psum(stats, "tp")
    return total[0], total[1]


def finish_norm(summed, sums, squares, gain, bias, width_total):
    center = sums / width_total
    spread = squares / width_total - center * center
    normed = (summed - center[:, None]) * lax.rsqrt(spread + EPS_LAYER)[:, None]
    return (normed * gain + bias).astype(jnp.bfloat16)


def body(
    residual,
    query_latent,
    shared_latent,
    rotary_key,
    query_gain,
    latent_gain,
    query_narrow,
    key_narrow,
    value_narrow,
    query_wide,
    key_wide,
    value_wide,
    output_narrow,
    output_wide,
    first_gain,
    first_bias,
    gate_weight,
    up_weight,
    down_weight,
    second_gain,
    second_bias,
):
    row_count = residual.shape[0]
    sp_count = lax.axis_size("sp")
    tp_count = lax.axis_size("tp")
    sp_index = lax.axis_index("sp").astype(jnp.uint32)
    tp_index = lax.axis_index("tp").astype(jnp.uint32)
    low = (sp_index >> 1) & 1

    part = row_count // tp_count
    part_at = tp_index * part
    own_latent = lax.dynamic_slice_in_dim(shared_latent, part_at, part, 0)
    own_rotary = lax.dynamic_slice_in_dim(rotary_key, part_at, part, 0)
    part_positions = (sp_index * row_count + part_at).astype(jnp.int32) + jnp.arange(
        part, dtype=jnp.int32
    )
    own_normed = root_scale(own_latent, latent_gain).astype(jnp.bfloat16)
    own_rotated = turn_axial(own_rotary.astype(jnp.float32)[:, None, :], part_positions)[
        :, 0, :
    ].astype(jnp.bfloat16)
    own_rows = jnp.concatenate([own_normed, own_rotated], axis=1)
    all_rows = lax.all_gather(own_rows, ("sp", "tp"), axis=0, tiled=True)

    half = gate_weight.shape[1] // 2

    def pack(which):
        gate_half = lax.dynamic_slice_in_dim(gate_weight, which * half, half, 1)
        up_half = lax.dynamic_slice_in_dim(up_weight, which * half, half, 1)
        return jnp.concatenate([gate_half, up_half], axis=1)

    pairs = (pack(low), pack(1 - low))
    downs = tuple(
        lax.dynamic_slice_in_dim(down_weight, which * half, half, 0) for which in (low, 1 - low)
    )
    feature_width = residual.shape[1]
    block_width = gate_weight.shape[0]
    ratio = jnp.uint32(feature_width // block_width)

    def spread(sources):
        found = {}
        for step in range(sp_count // 2):
            found[step * 2] = sources[0] if step == 0 else swap(sources[step % 2], "sp", step * 2)
            found[step * 2 + 1] = swap(found[step * 2], "sp", 1)
        return found

    gate_up_blocks = spread(pairs)
    down_blocks = spread(downs)

    def place(blocks, axis, shape):
        whole = jnp.zeros(shape, jnp.bfloat16)
        for step, block in blocks.items():
            index = sp_index ^ step
            at = (lax.div(index, ratio) ^ tp_index) * feature_width
            at = at + lax.rem(index, ratio) * block_width
            whole = lax.dynamic_update_slice_in_dim(whole, block, at, axis)
        return whole

    positions = (sp_index * row_count).astype(jnp.int32) + jnp.arange(row_count, dtype=jnp.int32)
    query_normed = root_scale(query_latent, query_gain).astype(jnp.bfloat16)
    narrow_queries = make_query(query_normed, query_narrow, NOPE_A, positions)
    wide_queries = make_query(query_normed, query_wide, NOPE_B, positions)
    narrow_heads = narrow_queries.shape[1]
    wide_heads = wide_queries.shape[1]
    kv_width = shared_latent.shape[1]
    normed = all_rows[:, :kv_width]
    rotated = all_rows[:, kv_width:]
    count = all_rows.shape[0]

    def up(weight, heads):
        made = jnp.dot(normed, weight, preferred_element_type=jnp.float32).astype(jnp.bfloat16)
        return made.reshape(count, heads, weight.shape[1] // heads)

    narrow_out = attend(
        narrow_queries,
        up(key_narrow, narrow_heads),
        up(value_narrow, narrow_heads),
        rotated,
        NOPE_A,
    )
    wide_out = attend(
        wide_queries, up(key_wide, wide_heads), up(value_wide, wide_heads), rotated, NOPE_B
    )
    attended = jnp.concatenate([narrow_out, wide_out], axis=1)
    output_weight = jnp.concatenate([output_narrow, output_wide], axis=0)
    terms = {}
    for q in range(tp_count):
        piece = lax.dynamic_slice_in_dim(
            output_weight, (tp_index ^ q) * feature_width, feature_width, 1
        )
        terms[q] = jnp.dot(attended, piece, preferred_element_type=jnp.float32)
    mixed = fold_tp(terms, tp_bits())[0]
    width_total = feature_width * tp_count
    summed = DEEP_ALPHA * residual.astype(jnp.float32) + mixed
    sums, squares = layer_stats(summed)
    normed_first = finish_norm(summed, sums, squares, first_gain, first_bias, width_total)

    mate_first = swap(normed_first, "sp", 2)
    own_blocks = gather_blocks(normed_first)
    mate_blocks = gather_blocks(mate_first)
    rows_in = jnp.concatenate(
        [
            jnp.concatenate([own_blocks[q] for q in range(tp_count)], axis=1),
            jnp.concatenate([mate_blocks[q] for q in range(tp_count)], axis=1),
        ],
        axis=0,
    )
    gate_up = place(gate_up_blocks, 0, (width_total, 2 * half))
    both = jnp.dot(rows_in, gate_up, preferred_element_type=jnp.float32)
    hidden = (jax.nn.silu(both[:, :half]) * both[:, half:]).astype(jnp.bfloat16)
    down = place(down_blocks, 1, (half, width_total))
    feed_terms = {
        q: jnp.dot(
            hidden,
            down[:, q * feature_width : (q + 1) * feature_width],
            preferred_element_type=jnp.float32,
        )
        for q in range(tp_count)
    }
    bits = tp_bits()
    feed_terms = fold_tp(feed_terms, bits[:-1])
    kept = sorted(feed_terms)
    packed = jnp.concatenate([feed_terms[q][row_count:].astype(jnp.bfloat16) for q in kept], axis=1)
    got = swap(packed, "sp", 2)
    feed_terms = {
        q: feed_terms[q][:row_count]
        + got[:, n * feature_width : (n + 1) * feature_width].astype(jnp.float32)
        for n, q in enumerate(kept)
    }
    feed = fold_tp(feed_terms, bits[-1:])[0]
    summed_two = DEEP_ALPHA * normed_first.astype(jnp.float32) + feed
    sums_two, squares_two = layer_stats(summed_two)
    return finish_norm(summed_two, sums_two, squares_two, second_gain, second_bias, width_total)


def solution(mesh):
    return jax.shard_map(
        body,
        mesh=mesh,
        in_specs=(
            P("sp", "tp"),
            P("sp", None),
            P("sp", None),
            P("sp", None),
            P(),
            P(),
            P(None, "tp"),
            P(None, "tp"),
            P(None, "tp"),
            P(None, "tp"),
            P(None, "tp"),
            P(None, "tp"),
            P("tp", None),
            P("tp", None),
            P("tp"),
            P("tp"),
            P("sp", "tp"),
            P("sp", "tp"),
            P("tp", "sp"),
            P("tp"),
            P("tp"),
        ),
        out_specs=P("sp", "tp"),
        check_vma=False,
    )
```

```python
import jax
import jax.numpy as jnp
from jax import lax
from jax.sharding import PartitionSpec as P

ROPE = 32
NOPE_A = 64
NOPE_B = 128
GRID_W = 64


EPS_ROOT = 1e-06
EPS_LAYER = 1e-05
THETA = 10000.0
DEEP_ALPHA = 2.0**0.25


def rotate(half_part, angle):
    lower, upper = jnp.split(half_part, 2, axis=-1)
    cosine = jnp.cos(angle)
    sine = jnp.sin(angle)
    return jnp.concatenate([lower * cosine - upper * sine, upper * cosine + lower * sine], axis=-1)


def turn_axial(values_in, positions):
    quarter = values_in.shape[-1] // 4
    freqs = THETA ** (-(2.0 * jnp.arange(quarter, dtype=jnp.float32)) / (2 * quarter))
    row_angle = (positions // GRID_W).astype(jnp.float32)[:, None, None] * freqs
    col_angle = (positions % GRID_W).astype(jnp.float32)[:, None, None] * freqs
    first_half, second_half = jnp.split(values_in, 2, axis=-1)
    return jnp.concatenate([rotate(first_half, row_angle), rotate(second_half, col_angle)], axis=-1)


def root_scale(latent, gain):
    floated = latent.astype(jnp.float32)
    return (
        floated * lax.rsqrt(jnp.mean(floated * floated, axis=-1, keepdims=True) + EPS_ROOT) * gain
    )


def make_query(normed, weight, plain_dim, positions):
    product = jnp.dot(normed, weight, preferred_element_type=jnp.float32)
    head_count = weight.shape[1] // (plain_dim + ROPE)
    product = product.reshape(product.shape[0], head_count, plain_dim + ROPE)
    turned = turn_axial(product[:, :, plain_dim:], positions)
    return jnp.concatenate([product[:, :, :plain_dim], turned], axis=-1).astype(jnp.bfloat16)


def attend(queries, keys, values, rotated, plain_dim):
    score_scale = queries.shape[2] ** (-0.5)
    scores = jnp.einsum(
        "qhd,khd->hqk", queries[:, :, :plain_dim], keys, preferred_element_type=jnp.float32
    )
    scores = scores + jnp.einsum(
        "qhd,kd->hqk", queries[:, :, plain_dim:], rotated, preferred_element_type=jnp.float32
    )
    scores = scores * score_scale
    largest = jnp.max(scores, axis=-1, keepdims=True)
    raised = jnp.exp(scores - largest)
    totals = jnp.sum(raised, axis=-1)
    weighted = jnp.einsum(
        "hqk,khd->qhd", raised.astype(jnp.bfloat16), values, preferred_element_type=jnp.float32
    )
    output = (weighted / totals.T[:, :, None]).astype(jnp.bfloat16)
    return output.reshape(output.shape[0], output.shape[1] * output.shape[2])


def swap(value, axis, bit):
    count = lax.axis_size(axis)
    return lax.ppermute(value, axis, [(i, i ^ bit) for i in range(count)])


def tp_bits():
    bits = []
    bit = 1
    while bit < lax.axis_size("tp"):
        bits.append(bit)
        bit *= 2
    return bits


def gather_blocks(own):
    blocks = {0: own}
    for bit in reversed(tp_bits()):
        for q in list(blocks):
            blocks[q ^ bit] = swap(blocks[q], "tp", bit)
    return blocks


def fold_tp(blocks, bits):
    for bit in bits:
        sent = [q for q in sorted(blocks) if q & bit]
        packed = jnp.concatenate([blocks[q].astype(jnp.bfloat16) for q in sent], axis=1)
        got = swap(packed, "tp", bit)
        width = got.shape[1] // len(sent)
        blocks = {
            q ^ bit: blocks[q ^ bit]
            + got[:, n * width : (n + 1) * width].astype(jnp.float32)
            for n, q in enumerate(sent)
        }
    return blocks


def layer_stats(summed):
    stats = jnp.stack([jnp.sum(summed, axis=1), jnp.sum(summed * summed, axis=1)])
    total = lax.psum(stats, "tp")
    return total[0], total[1]


def finish_norm(summed, sums, squares, gain, bias, width_total):
    center = sums / width_total
    spread = squares / width_total - center * center
    normed = (summed - center[:, None]) * lax.rsqrt(spread + EPS_LAYER)[:, None]
    return (normed * gain + bias).astype(jnp.bfloat16)


def body(
    residual,
    query_latent,
    shared_latent,
    rotary_key,
    query_gain,
    latent_gain,
    query_narrow,
    key_narrow,
    value_narrow,
    query_wide,
    key_wide,
    value_wide,
    output_narrow,
    output_wide,
    first_gain,
    first_bias,
    gate_weight,
    up_weight,
    down_weight,
    second_gain,
    second_bias,
):
    row_count = residual.shape[0]
    sp_count = lax.axis_size("sp")
    tp_count = lax.axis_size("tp")
    sp_index = lax.axis_index("sp").astype(jnp.uint32)
    tp_index = lax.axis_index("tp").astype(jnp.uint32)
    low = (sp_index >> 1) & 1

    part = row_count // tp_count
    part_at = tp_index * part
    own_latent = lax.dynamic_slice_in_dim(shared_latent, part_at, part, 0)
    own_rotary = lax.dynamic_slice_in_dim(rotary_key, part_at, part, 0)
    part_positions = (sp_index * row_count + part_at).astype(jnp.int32) + jnp.arange(
        part, dtype=jnp.int32
    )
    own_normed = root_scale(own_latent, latent_gain).astype(jnp.bfloat16)
    own_rotated = turn_axial(own_rotary.astype(jnp.float32)[:, None, :], part_positions)[
        :, 0, :
    ].astype(jnp.bfloat16)
    own_rows = jnp.concatenate([own_normed, own_rotated], axis=1)
    all_rows = jnp.concatenate([own_rows, swap(own_rows, "sp", 1)], axis=0)
    found = [all_rows]
    for step in range(1, sp_count // 2):
        found.append(swap(all_rows, "sp", step * 2))
    all_rows = jnp.concatenate(found, axis=0)
    for bit in reversed(tp_bits()):
        all_rows = jnp.concatenate([all_rows, swap(all_rows, "tp", bit)], axis=0)

    half = gate_weight.shape[1] // 2

    def pack(which):
        gate_half = lax.dynamic_slice_in_dim(gate_weight, which * half, half, 1)
        up_half = lax.dynamic_slice_in_dim(up_weight, which * half, half, 1)
        return jnp.concatenate([gate_half, up_half], axis=1)

    pairs = (pack(low), pack(1 - low))
    downs = tuple(
        lax.dynamic_slice_in_dim(down_weight, which * half, half, 0) for which in (low, 1 - low)
    )
    feature_width = residual.shape[1]
    block_width = gate_weight.shape[0]
    ratio = jnp.uint32(feature_width // block_width)

    def spread(sources):
        found = {}
        for step in range(sp_count // 2):
            found[step * 2] = sources[0] if step == 0 else swap(sources[step % 2], "sp", step * 2)
            found[step * 2 + 1] = swap(found[step * 2], "sp", 1)
        return found

    gate_up_blocks = spread(pairs)
    down_blocks = spread(downs)

    def place(blocks, axis, shape):
        whole = jnp.zeros(shape, jnp.bfloat16)
        for step, block in blocks.items():
            index = sp_index ^ step
            at = (lax.div(index, ratio) ^ tp_index) * feature_width
            at = at + lax.rem(index, ratio) * block_width
            whole = lax.dynamic_update_slice_in_dim(whole, block, at, axis)
        return whole

    positions = (sp_index * row_count).astype(jnp.int32) + jnp.arange(row_count, dtype=jnp.int32)
    query_normed = root_scale(query_latent, query_gain).astype(jnp.bfloat16)
    narrow_queries = make_query(query_normed, query_narrow, NOPE_A, positions)
    wide_queries = make_query(query_normed, query_wide, NOPE_B, positions)
    narrow_heads = narrow_queries.shape[1]
    wide_heads = wide_queries.shape[1]
    kv_width = shared_latent.shape[1]
    normed = all_rows[:, :kv_width]
    rotated = all_rows[:, kv_width:]
    count = all_rows.shape[0]

    def up(weight, heads):
        made = jnp.dot(normed, weight, preferred_element_type=jnp.float32).astype(jnp.bfloat16)
        return made.reshape(count, heads, weight.shape[1] // heads)

    narrow_out = attend(
        narrow_queries,
        up(key_narrow, narrow_heads),
        up(value_narrow, narrow_heads),
        rotated,
        NOPE_A,
    )
    wide_out = attend(
        wide_queries, up(key_wide, wide_heads), up(value_wide, wide_heads), rotated, NOPE_B
    )
    attended = jnp.concatenate([narrow_out, wide_out], axis=1)
    output_weight = jnp.concatenate([output_narrow, output_wide], axis=0)
    terms = {}
    for q in range(tp_count):
        piece = lax.dynamic_slice_in_dim(
            output_weight, (tp_index ^ q) * feature_width, feature_width, 1
        )
        terms[q] = jnp.dot(attended, piece, preferred_element_type=jnp.float32)
    mixed = fold_tp(terms, tp_bits())[0]
    width_total = feature_width * tp_count
    summed = DEEP_ALPHA * residual.astype(jnp.float32) + mixed
    sums, squares = layer_stats(summed)
    normed_first = finish_norm(summed, sums, squares, first_gain, first_bias, width_total)

    mate_first = swap(normed_first, "sp", 2)
    own_blocks = gather_blocks(normed_first)
    mate_blocks = gather_blocks(mate_first)
    rows_in = jnp.concatenate(
        [
            jnp.concatenate([own_blocks[q] for q in range(tp_count)], axis=1),
            jnp.concatenate([mate_blocks[q] for q in range(tp_count)], axis=1),
        ],
        axis=0,
    )
    gate_up = place(gate_up_blocks, 0, (width_total, 2 * half))
    both = jnp.dot(rows_in, gate_up, preferred_element_type=jnp.float32)
    hidden = (jax.nn.silu(both[:, :half]) * both[:, half:]).astype(jnp.bfloat16)
    down = place(down_blocks, 1, (half, width_total))
    bits = tp_bits()

    def feed_half(rows):
        made = {
            q: jnp.dot(
                rows,
                down[:, q * feature_width : (q + 1) * feature_width],
                preferred_element_type=jnp.float32,
            )
            for q in range(tp_count)
        }
        return fold_tp(made, bits[:-1])

    mate_terms = feed_half(hidden[row_count:])
    kept = sorted(mate_terms)
    packed = jnp.concatenate([mate_terms[q].astype(jnp.bfloat16) for q in kept], axis=1)
    got = swap(packed, "sp", 2)
    own_terms = feed_half(hidden[:row_count])
    feed_terms = {
        q: own_terms[q]
        + got[:, n * feature_width : (n + 1) * feature_width].astype(jnp.float32)
        for n, q in enumerate(kept)
    }
    feed = fold_tp(feed_terms, bits[-1:])[0]
    summed_two = DEEP_ALPHA * normed_first.astype(jnp.float32) + feed
    sums_two, squares_two = layer_stats(summed_two)
    return finish_norm(summed_two, sums_two, squares_two, second_gain, second_bias, width_total)


def solution(mesh):
    return jax.shard_map(
        body,
        mesh=mesh,
        in_specs=(
            P("sp", "tp"),
            P("sp", None),
            P("sp", None),
            P("sp", None),
            P(),
            P(),
            P(None, "tp"),
            P(None, "tp"),
            P(None, "tp"),
            P(None, "tp"),
            P(None, "tp"),
            P(None, "tp"),
            P("tp", None),
            P("tp", None),
            P("tp"),
            P("tp"),
            P("sp", "tp"),
            P("sp", "tp"),
            P("tp", "sp"),
            P("tp"),
            P("tp"),
        ),
        out_specs=P("sp", "tp"),
        check_vma=False,
    )
```
